32 devices in a mesh: grp: 2 (over x), sp: 4 (over y, core), tp: 4 (over z).
Axes of the slice: x: 2, y: 2, z: 4, core: 2. Of those that a mesh axis runs over, the one named last changes fastest.
Arguments:
- residual: bfloat16 [4096, 2048], P(('grp', 'sp', 'tp')), parts along dimension 0, may hold values from -6 to 6
- grouped_value_heads: bfloat16 [4096, 2, 1024], P(('grp', 'sp'), None, 'tp'), parts along dimension 0, may hold values from -6 to 6
- output_gate_heads: bfloat16 [4096, 2, 1024], P(('grp', 'sp'), None, 'tp'), parts along dimension 0, may hold values from -6 to 6
- projected_key_query: bfloat16 [4096, 384], P(('grp', 'sp')), parts along dimension 0, may hold values from -6 to 6
- raw_step_size: bfloat16 [4096, 2, 16], P(('grp', 'sp'), None, 'tp'), parts along dimension 0, may hold values from -3 to 3
- step_size_bias: float32 [2, 16], P(None, 'tp'), may hold values from -1 to 0.5
- head_decay_logarithm: float32 [2, 16], P(None, 'tp'), may hold values from -16 to -2
- position_extra_decay: float32 [4096], P(('grp', 'sp')), parts along dimension 0, may hold values from -0.7 to 0
- head_skip_weight: float32 [2, 16], P(None, 'tp'), may hold values from 0.5 to 2
- value_kernel_taps: bfloat16 [4, 2, 1024], P(None, None, 'tp'), may hold values from -3 to 3
- key_query_kernel: bfloat16 [4, 384], replicated, may hold values from -3 to 3
- head_norm_gain: float32 [2, 1024], P(None, 'tp'), may hold values from 0.1 to 1.9
- output_matrix: bfloat16 [2, 1024, 2048], P(None, 'tp'), may hold values from -0.125 to 0.125
- expert_norm_gain: float32 [2048], replicated, may hold values from 0.1 to 1.9
- expert_gate_weight: bfloat16 [4, 2048, 4096], P('sp', None, 'tp'), may hold values from -0.125 to 0.125
- expert_up_weight: bfloat16 [4, 2048, 4096], P('sp', None, 'tp'), may hold values from -0.125 to 0.125
- expert_down_weight: bfloat16 [4, 4096, 2048], P('sp', 'tp'), may hold values from -0.09375 to 0.09375
- token_expert_choice: int32 [4096, 2], P(('grp', 'sp', 'tp')), parts along dimension 0, may hold values from 0 to 3, all different within a row; in each aligned block of 128 rows (0 to 127, 128 to 255, ...) at most 65 rows name the same one
- expert_output_weight: float32 [4096, 2], P(('grp', 'sp', 'tp')), parts along dimension 0, may hold values from 0.2 to 1
Outputs:
- layer_out: bfloat16 [4096, 2048], P(('grp', 'sp', 'tp')), parts along dimension 0
The draws below stay inside these ranges and needn't reach their ends.
There are 2 independent parts, one for each index of `grp`. The reference program is written for one: setup_inputs(seed, part) draws one part's arguments, and reference() takes and returns one part's arrays. A program takes and returns all parts, laid end to end along the dimension named above; an argument that names none is the same for every part. Nothing has to cross between parts.
Inputs may be any that keep to these rules, and one draw needn't show every extreme that they name: `token_expert_choice`: each row names two different experts. The token rows of one device name one expert at most 65 times.
All inputs are finite; a program needn't handle non-finite values.
Results may differ from the reference program's by a relative error of at most 0.015.
Values may be sent and summed in bfloat16 or wider, within the bound.
A program may use at most 128 MiB of HBM per device.

```python
import math
import jax
import jax.numpy as jnp
import numpy as np
from jax import lax

D = 2048
FF = 4096
GROUP_HEADS = 16
HEAD_DIM = 64
STATE_ONE = 64
STATE_TWO = 128
TAPS = 4
BLOCK = 128
ROWS_DEV = 128
SEQ_DEV = 512
TOKENS = 2048
EXPERTS = 4
CAP = 65
N_TP = 4


def draw_raw_step_size(key, part):
    first, second, third = jax.random.split(jax.random.fold_in(key, 11), 3)
    segments = TOKENS // SEQ_DEV
    blocks = TOKENS // BLOCK
    segment_shift = jax.random.uniform(first, (segments, 1), jnp.float32, -1.0, 1.0)
    segment_shift = jnp.repeat(segment_shift, SEQ_DEV // BLOCK, axis=0)
    block_shift = jax.random.uniform(second, (blocks, 1), jnp.float32, -0.5, 0.5)
    grid_shape = (blocks, BLOCK * 2 * GROUP_HEADS)
    jitter = jnp.clip(0.6 * jax.random.normal(third, grid_shape, jnp.float32), -1.5, 1.5)
    return (segment_shift + block_shift + jitter).reshape(TOKENS, 2, GROUP_HEADS).astype(jnp.bfloat16)


def draw_head_decay_logarithm(key, part):
    first, second = jax.random.split(jax.random.fold_in(key, 23))
    slow_share = 0.5
    choose_slow = jax.random.uniform(first, (2, GROUP_HEADS), jnp.float32) < slow_share
    level = jax.random.uniform(second, (2, GROUP_HEADS), jnp.float32, 0.0, 1.0)
    slow_rate = jnp.log(0.3 / TOKENS) + level * jnp.log(5.0)
    fast_rate = jnp.log(0.03) + level * jnp.log(3.0)
    return jnp.where(choose_slow, slow_rate, fast_rate).astype(jnp.float32)


def draw_position_extra_decay(key, part):
    first, second = jax.random.split(jax.random.fold_in(key, 37))
    spots = jax.random.randint(first, (3,), 0, TOKENS)
    depth = jax.random.uniform(second, (3,), jnp.float32, jnp.log(0.5), jnp.log(0.8))
    places = jnp.arange(TOKENS)
    struck = places[:, None] == spots[None, :]
    return jnp.sum(jnp.where(struck, depth[None, :], 0.0), axis=1).astype(jnp.float32)


def block_levels(stream_key, extent, cuts, least, largest):
    def one(axis_at, blocks):
        steps = jax.random.uniform(jax.random.fold_in(jax.random.fold_in(stream_key, 6), axis_at), (blocks,), jnp.float32, least / len(cuts), largest / len(cuts))
        return jnp.repeat(jnp.exp(steps), extent[axis_at] // blocks).reshape((-1,) + (1,) * (len(extent) - axis_at - 1))

    loudness = one(*cuts[0])
    for cut in cuts[1:]:
        loudness = loudness * one(*cut)
    return loudness


def deal_out(own_key, own, number, rows, number_of, top, reach, lean):
    ranking = jax.random.permutation(own_key, number_of)
    heavy_load, ordinary = load_shares(number_of, rows * top, reach, lean, True), load_shares(number_of, rows * top, reach, lean, False)
    places = jnp.arange(number_of)

    def named(lengths, turn):
        used = int((lengths > 0).sum())
        fixed = max(1, used // 4)
        passed = fixed + (places - fixed + turn * (used - fixed)) % max(1, number_of - fixed)
        return jnp.zeros((number_of,), jnp.int32).at[ranking[jnp.where(places < fixed, places, passed)]].set(jnp.asarray(lengths, jnp.int32))

    lengths = jnp.where(number % 4 == 0, named(heavy_load, number // 4), named(ordinary, number - number // 4 - 1))
    mixed = jax.random.permutation(jax.random.fold_in(own, 3), number_of)
    donor, receiver = mixed[0:number_of // 2 * 2:2], mixed[1:number_of // 2 * 2:2]
    margin = jnp.minimum(lengths[donor] - 1, reach - lengths[receiver]) // 2
    margin = jnp.where((donor == ranking[0]) | (receiver == ranking[0]) | (lengths[receiver] == 0), 0, jnp.maximum(margin, 0))
    passed = jax.random.randint(jax.random.fold_in(own, 4), (number_of // 2,), 0, 1 << 20) % (margin + 1)
    lengths = lengths.at[donor].add(-passed).at[receiver].add(passed)
    items = jnp.searchsorted(jnp.cumsum(lengths), jnp.arange(rows * top), side="right").astype(jnp.int32)
    grid = items.reshape(top, rows).T
    grid = grid[jax.random.permutation(jax.random.fold_in(own, 1), rows)]
    turn = jax.random.randint(jax.random.fold_in(own, 2), (rows, 1), 0, top)
    return jnp.take_along_axis(grid, (jnp.arange(top)[None, :] + turn) % top, axis=1)


def load_shares(count, total, bound, lean, full):
    weights = [(1 << 20) // math.isqrt(standing ** lean) + 1 for standing in range(1, count + 1)]
    largest = bound if full else min(bound, max(-(-total // count), total * weights[0] // sum(weights)))
    least = 1 if total - largest >= count - 1 else 0
    holding, surplus = [largest] + [least] * (count - 1), total - largest - least * (count - 1)
    while surplus > 0:
        candidates = [i for i in range(1, count) if holding[i] < largest] or [i for i in range(1, count) if holding[i] < bound]
        whole, remaining = sum([weights[i] for i in candidates]), surplus
        for i in candidates:
            extra = min(bound - holding[i], max(1, remaining * weights[i] // whole), surplus)
            holding[i] = holding[i] + extra
            surplus = surplus - extra
    return np.array(holding)


def centred(own_key, shape, deviation, bound, shards=(), kind=jnp.bfloat16):
    entries = jax.random.normal(own_key, shape, jnp.float32) * deviation
    if len(shards) > 0:
        entries = block_levels(own_key, shape, shards, -0.22, 0.18) * entries
    return jnp.clip(entries, min=-bound, max=bound).astype(kind)


def setup_inputs(seed: int = 0, part: int = 0) -> dict:
    arg_keys = jax.random.split(jax.random.key(seed), 20)
    own_keys = jax.random.split(jax.random.fold_in(arg_keys[19], part), 20)
    residual = centred(own_keys[0], (TOKENS, D), 1.0, 6.0, ((0, 16),))
    grouped_value_heads = centred(own_keys[1], (TOKENS, 2, GROUP_HEADS * HEAD_DIM), 1.0, 6.0, ((0, 4), (2, 4)))
    output_gate_heads = centred(own_keys[2], (TOKENS, 2, GROUP_HEADS * HEAD_DIM), 1.0, 6.0, ((0, 4), (2, 4)))
    projected_key_query = centred(own_keys[3], (TOKENS, 2 * STATE_ONE + 2 * STATE_TWO), 1.0, 6.0, ((0, 4),))
    raw_step_size = draw_raw_step_size(jax.random.fold_in(jax.random.fold_in(arg_keys[19], part), 71), part)
    step_size_bias = jnp.clip(-1.0 + 1.5 * jax.random.uniform(arg_keys[5], (2, GROUP_HEADS), jnp.float32) ** block_levels(arg_keys[5], (2, GROUP_HEADS), ((1, 4),), -0.2, 0.2), -1.0, 0.5)
    head_decay_logarithm = draw_head_decay_logarithm(jax.random.fold_in(arg_keys[19], 71), part)
    position_extra_decay = draw_position_extra_decay(jax.random.fold_in(jax.random.fold_in(arg_keys[19], part), 71), part)
    head_skip_weight = jnp.clip(0.5 + 1.5 * jax.random.uniform(arg_keys[8], (2, GROUP_HEADS), jnp.float32) ** block_levels(arg_keys[8], (2, GROUP_HEADS), ((1, 4),), -0.2, 0.2), 0.5, 2.0)
    value_kernel_taps = centred(arg_keys[9], (TAPS, 2, GROUP_HEADS * HEAD_DIM), 0.5, 3.0, ((2, 4),))
    key_query_kernel = centred(arg_keys[10], (TAPS, 2 * STATE_ONE + 2 * STATE_TWO), 0.5, 3.0)
    head_norm_gain = jnp.clip(1.0 + 0.18 * jax.random.normal(arg_keys[11], (2, GROUP_HEADS * HEAD_DIM), jnp.float32), 0.1, 1.9)
    output_matrix = centred(arg_keys[12], (2, GROUP_HEADS * HEAD_DIM, D), (2 * GROUP_HEADS * HEAD_DIM) ** -0.5, 0.125, ((1, 4),))
    expert_norm_gain = jnp.clip(1.0 + 0.18 * jax.random.normal(arg_keys[13], (D,), jnp.float32), 0.1, 1.9)
    expert_gate_weight = centred(arg_keys[14], (EXPERTS, D, FF), D ** -0.5, 0.125, ((0, 4), (2, 4)))
    expert_up_weight = centred(arg_keys[15], (EXPERTS, D, FF), D ** -0.5, 0.125, ((0, 4), (2, 4)))
    expert_down_weight = centred(arg_keys[16], (EXPERTS, FF, D), FF ** -0.5, 0.09375, ((0, 4), (1, 4)))
    token_expert_choice_keys = jax.random.split(jax.random.fold_in(own_keys[17], 1), TOKENS // ROWS_DEV)
    token_expert_choice_turns = jax.random.permutation(jax.random.fold_in(own_keys[17], 3), TOKENS // ROWS_DEV)
    token_expert_choice = jax.vmap(lambda own, number: deal_out(jax.random.fold_in(own_keys[17], 2), own, number, ROWS_DEV, EXPERTS, 2, CAP, 1))(token_expert_choice_keys, token_expert_choice_turns).reshape((TOKENS, 2))
    expert_output_weight = jnp.clip(0.2 + 0.8 * jax.random.uniform(own_keys[18], (TOKENS, 2), jnp.float32) ** block_levels(own_keys[18], (TOKENS, 2), ((0, 16),), -0.2, 0.2), 0.2, 1.0)
    return dict(residual=residual, grouped_value_heads=grouped_value_heads, output_gate_heads=output_gate_heads, projected_key_query=projected_key_query, raw_step_size=raw_step_size, step_size_bias=step_size_bias, head_decay_logarithm=head_decay_logarithm, position_extra_decay=position_extra_decay, head_skip_weight=head_skip_weight, value_kernel_taps=value_kernel_taps, key_query_kernel=key_query_kernel, head_norm_gain=head_norm_gain, output_matrix=output_matrix, expert_norm_gain=expert_norm_gain, expert_gate_weight=expert_gate_weight, expert_up_weight=expert_up_weight, expert_down_weight=expert_down_weight, token_expert_choice=token_expert_choice, expert_output_weight=expert_output_weight)


EPSILON = 1e-06

def causal_conv(signal, tap_weights):
    tap_count = tap_weights.shape[0]
    length = signal.shape[0]
    padded = jnp.pad(signal, ((tap_count - 1, 0), (0, 0)))
    summed = jnp.zeros((length, signal.shape[1]), jnp.float32)
    for offset in range(tap_count):
        summed = summed + padded[offset:offset + length].astype(jnp.float32) * tap_weights[offset].astype(jnp.float32)
    return summed

def advance(carried, pair_item):
    block_state, fading_step = pair_item
    return (carried * fading_step[:, None, None] + block_state, carried)

def group_scan(value_rows, key_rows, query_rows, step_spacing, decay_logarithm, block_size):
    positions, head_count, head_width = value_rows.shape
    block_count = positions // block_size
    value_rows = value_rows.reshape(block_count, block_size, head_count, head_width).astype(jnp.float32)
    key_rows = key_rows.reshape(block_count, block_size, key_rows.shape[-1]).astype(jnp.float32)
    query_rows = query_rows.reshape(block_count, block_size, query_rows.shape[-1]).astype(jnp.float32)
    step_spacing = step_spacing.reshape(block_count, block_size, head_count)
    running = jnp.cumsum(decay_logarithm.reshape(block_count, block_size, head_count), axis=1)
    scores = jnp.einsum('kln,ksn->kls', query_rows, key_rows)
    causal = jnp.tril(jnp.ones((block_size, block_size), jnp.bool_))
    spread = running[:, :, None, :] - running[:, None, :, :]
    damping = jnp.exp(jnp.where(causal[None, :, :, None], spread, -jnp.inf))
    weights = (scores[:, :, :, None] * damping * step_spacing[:, None, :, :]).astype(jnp.bfloat16)
    near_part = jnp.einsum('klsh,kshp->klhp', weights.astype(jnp.float32), value_rows)
    fading = jnp.exp(running[:, -1:, :] - running) * step_spacing
    scaled_keys = (key_rows[:, :, None, :] * fading[:, :, :, None]).astype(jnp.bfloat16)
    states = jnp.einsum('kshn,kshp->khpn', scaled_keys.astype(jnp.float32), value_rows)
    anchor = jnp.zeros(states.shape[1:], jnp.float32)
    last_state, entering = lax.scan(advance, anchor, (states, jnp.exp(running[:, -1, :])))
    far_part = jnp.einsum('kln,khpn->klhp', query_rows, entering, precision=lax.Precision.HIGHEST)
    far_part = far_part * jnp.exp(running)[:, :, :, None]
    return (near_part + far_part).reshape(positions, head_count, head_width)

def reference(residual, grouped_value_heads, output_gate_heads, projected_key_query, raw_step_size, step_size_bias, head_decay_logarithm, position_extra_decay, head_skip_weight, value_kernel_taps, key_query_kernel, head_norm_gain, output_matrix, expert_norm_gain, expert_gate_weight, expert_up_weight, expert_down_weight, token_expert_choice, expert_output_weight):
    lane_count = 2 * GROUP_HEADS * HEAD_DIM
    flat_values = grouped_value_heads.reshape(TOKENS, lane_count)
    conv_heads = jax.nn.silu(causal_conv(flat_values, value_kernel_taps.reshape(TAPS, lane_count))).astype(jnp.bfloat16)
    conv_rows = jax.nn.silu(causal_conv(projected_key_query, key_query_kernel)).astype(jnp.bfloat16)
    step_spacing = jax.nn.softplus(raw_step_size.astype(jnp.float32) + step_size_bias[None])
    decay_logarithm = position_extra_decay[:, None, None] - jnp.exp(head_decay_logarithm)[None] * step_spacing
    value_heads = conv_heads.reshape(TOKENS, 2, GROUP_HEADS, HEAD_DIM)
    bounds = [0, STATE_ONE, 2 * STATE_ONE, 2 * STATE_ONE + STATE_TWO, 2 * STATE_ONE + 2 * STATE_TWO]
    group_parts = []
    for group_index in range(2):
        key_rows = conv_rows[:, bounds[2 * group_index]:bounds[2 * group_index + 1]]
        query_rows = conv_rows[:, bounds[2 * group_index + 1]:bounds[2 * group_index + 2]]
        group_parts.append(group_scan(value_heads[:, group_index], key_rows, query_rows, step_spacing[:, group_index], decay_logarithm[:, group_index], BLOCK))
    mixer_sum = jnp.stack(group_parts, axis=1) + head_skip_weight[None, :, :, None] * value_heads.astype(jnp.float32)
    gated_rows = mixer_sum * jax.nn.silu(output_gate_heads.astype(jnp.float32).reshape(TOKENS, 2, GROUP_HEADS, HEAD_DIM))
    scale_rows = lax.rsqrt(lax.optimization_barrier(jnp.mean(gated_rows * gated_rows, axis=3, keepdims=True)) + EPSILON)
    mixed_heads = (gated_rows * scale_rows * head_norm_gain.reshape(2, GROUP_HEADS, HEAD_DIM)).astype(jnp.bfloat16)
    mix_out = jnp.dot(mixed_heads.reshape(TOKENS, lane_count), output_matrix.reshape(lane_count, D), preferred_element_type=jnp.float32)
    stream = (residual.astype(jnp.float32) + mix_out).astype(jnp.bfloat16)
    wide_stream = stream.astype(jnp.float32)
    normed = (wide_stream * lax.rsqrt(lax.optimization_barrier(jnp.mean(wide_stream * wide_stream, axis=1, keepdims=True)) + EPSILON) * expert_norm_gain[None]).astype(jnp.bfloat16)
    sources = TOKENS // ROWS_DEV
    flat_ids = token_expert_choice.reshape(sources, 2 * ROWS_DEV)
    matches = (flat_ids[:, :, None] == jnp.arange(EXPERTS, dtype=jnp.int32)[None, None, :]).astype(jnp.int32)
    slot_rank = lax.optimization_barrier(jnp.sum((jnp.cumsum(matches, axis=1) - matches) * matches, axis=2))
    column = jnp.arange(sources, dtype=jnp.int32)[:, None] * CAP + slot_rank
    token_index = jnp.repeat(jnp.arange(TOKENS, dtype=jnp.int32).reshape(sources, ROWS_DEV), 2, axis=1)
    slot_table = jnp.zeros((EXPERTS, sources * CAP), jnp.int32).at[flat_ids.reshape(-1), column.reshape(-1)].set(token_index.reshape(-1))
    slice_width = FF // N_TP

    def one_expert(expert_index):
        gathered = jnp.take(normed, slot_table[expert_index], axis=0)
        gate_out = jnp.dot(gathered, expert_gate_weight[expert_index], preferred_element_type=jnp.float32)
        up_out = jnp.dot(gathered, expert_up_weight[expert_index], preferred_element_type=jnp.float32)
        hidden = (jax.nn.silu(gate_out) * up_out).astype(jnp.bfloat16)
        sliced = hidden.reshape(gathered.shape[0], N_TP, slice_width).astype(jnp.float32)
        down_slices = expert_down_weight[expert_index].reshape(N_TP, slice_width, D).astype(jnp.float32)
        pieces = jnp.einsum('rtf,tfd->rtd', sliced, down_slices).astype(jnp.bfloat16)
        pieces = lax.optimization_barrier(pieces).astype(jnp.float32)
        return lax.optimization_barrier(jnp.sum(pieces, axis=1)).astype(jnp.bfloat16)
    outputs = lax.map(one_expert, jnp.arange(EXPERTS, dtype=jnp.int32))
    picked = outputs[flat_ids.reshape(-1), column.reshape(-1)].reshape(TOKENS, 2, D).astype(jnp.float32)
    weighted = expert_output_weight[:, 0:1] * picked[:, 0] + expert_output_weight[:, 1:2] * picked[:, 1]
    return (wide_stream + weighted).astype(jnp.bfloat16)
```

```python
import jax
import jax.numpy as jnp
from jax import lax
from jax.experimental import pallas as pl
from jax.experimental.pallas import tpu as pltpu
from jax.sharding import PartitionSpec as P

HEAD_DIM = 64
STATE_ONE = 64
STATE_TWO = 128
BLOCK = 128


EPSILON = 1e-06


def passed_along(shard, axis, by):
    length = lax.axis_size(axis)
    pairs = [(i, i + by) for i in range(length) if 0 <= i + by < length]
    return lax.ppermute(shard, axis, pairs)


HIGHEST = lax.Precision.HIGHEST
PACK_ROWS = 16


def full_dot(left, right):
    return jnp.dot(left, right, precision=HIGHEST, preferred_element_type=jnp.float32)


def spread_matrix(head_count):
    shape = (head_count, head_count * HEAD_DIM)
    rows = lax.broadcasted_iota(jnp.int32, shape, 0)
    lanes = lax.broadcasted_iota(jnp.int32, shape, 1)
    return (lanes // HEAD_DIM == rows).astype(jnp.float32)


def silu(value):
    return value * (1.0 / (1.0 + jnp.exp(-value)))


def state_kernel(
    value_ref, key_ref, prior_ref, raw_ref, bias_ref, rate_ref, extra_ref, value_taps_ref,
    key_taps_ref, conv_ref, conv_key_ref, running_ref, spacing_ref, states_ref, pack_ref, pad_ref,
):
    positions, lanes = value_ref.shape
    taps = value_taps_ref.shape[0]
    half = lanes // 2
    pad_ref[8 - taps + 1 : 8, :] = prior_ref[...].astype(jnp.float32)
    pad_ref[8:, :lanes] = value_ref[...].astype(jnp.float32)
    pad_ref[8:, lanes:] = key_ref[...].astype(jnp.float32)
    spacing = jax.nn.softplus(raw_ref[...].astype(jnp.float32) + bias_ref[...])
    log_decay = extra_ref[...] - jnp.exp(rate_ref[...]) * spacing
    spacing_ref[...] = spacing
    head_count = spacing.shape[1]
    spread = spread_matrix(head_count)
    row = lax.broadcasted_iota(jnp.int32, (BLOCK, BLOCK), 0)
    col = lax.broadcasted_iota(jnp.int32, (BLOCK, BLOCK), 1)
    tril = (row >= col).astype(jnp.float32)
    carried = [jnp.zeros((STATE_ONE, half), jnp.float32), jnp.zeros((STATE_TWO, half), jnp.float32)]
    total = jnp.zeros((1, lanes), jnp.float32)
    starts = (0, 2 * STATE_ONE)
    sizes = (STATE_ONE, STATE_TWO)
    value_taps = value_taps_ref[...].astype(jnp.float32)
    key_taps = key_taps_ref[...].astype(jnp.float32)
    for block in range(positions // BLOCK):
        lo = block * BLOCK
        summed = jnp.zeros((BLOCK, lanes), jnp.float32)
        key_sum = jnp.zeros((BLOCK, key_ref.shape[1]), jnp.float32)
        for tap in range(taps):
            at = lo + 8 - taps + 1 + tap
            summed = summed + pad_ref[at : at + BLOCK, :lanes] * value_taps[tap : tap + 1]
            key_sum = key_sum + pad_ref[at : at + BLOCK, lanes:] * key_taps[tap : tap + 1]
        conv = silu(summed).astype(jnp.bfloat16)
        conv_key = silu(key_sum).astype(jnp.bfloat16)
        conv_ref[lo : lo + BLOCK, :] = conv
        conv_key_ref[lo : lo + BLOCK, :] = conv_key
        running = full_dot(tril, log_decay[lo : lo + BLOCK])
        running_ref[lo : lo + BLOCK, :] = running
        end = running[BLOCK - 1 : BLOCK]
        fading = jnp.exp(end - running) * spacing[lo : lo + BLOCK]
        scaled = (conv.astype(jnp.float32) * full_dot(fading, spread)).astype(jnp.bfloat16)
        wide_end = full_dot(jnp.broadcast_to(end, (8, head_count)), spread)[:1]
        total = total + wide_end
        fade = jnp.exp(wide_end)
        for group in range(2):
            keys = conv_key[:, starts[group] : starts[group] + sizes[group]]
            at = group * STATE_ONE
            states_ref[block, at : at + sizes[group], :] = carried[group]
            state = lax.dot_general(
                keys,
                scaled[:, group * half : (group + 1) * half],
                (((0,), (0,)), ((), ())),
                preferred_element_type=jnp.float32,
            )
            carried[group] = carried[group] * fade[:, group * half : (group + 1) * half] + state
    pack_ref[:STATE_ONE, :] = carried[0].astype(jnp.bfloat16)
    pack_ref[STATE_ONE : STATE_ONE + STATE_TWO, :] = carried[1].astype(jnp.bfloat16)
    high = total.astype(jnp.bfloat16).astype(jnp.float32)
    low = total - high
    line = lax.broadcasted_iota(jnp.int32, (PACK_ROWS, half), 0)
    packed = jnp.zeros((PACK_ROWS, half), jnp.float32)
    for at, piece in enumerate((high[:, :half], high[:, half:], low[:, :half], low[:, half:])):
        packed = jnp.where(line == at, piece, packed)
    pack_ref[STATE_ONE + STATE_TWO :, :] = packed.astype(jnp.bfloat16)


def mix_kernel(
    place_ref, conv_ref, key_ref, running_ref, spacing_ref, states_ref, packs_ref, gate_ref,
    skip_ref, gain_ref, matrix_ref, out_ref, entered_ref, reach_ref,
):
    block = pl.program_id(0)
    lanes = conv_ref.shape[1]
    half = lanes // 2
    depth = STATE_ONE + STATE_TWO
    head_count = spacing_ref.shape[1]
    spread = spread_matrix(head_count)

    @pl.when(block == 0)
    def _():
        reach_ref[...] = jnp.zeros_like(reach_ref)
        entered_ref[...] = jnp.zeros_like(entered_ref)
        for source in range(packs_ref.shape[0] - 1):

            @pl.when(source < place_ref[0])
            def _():
                decay = packs_ref[source, depth:, :].astype(jnp.float32)
                one = jnp.exp(decay[0:1] + decay[2:3])
                two = jnp.exp(decay[1:2] + decay[3:4])
                entered_ref[:STATE_ONE, :] = entered_ref[:STATE_ONE, :] * one + packs_ref[
                    source, :STATE_ONE, :
                ].astype(jnp.float32)
                entered_ref[STATE_ONE:, :] = entered_ref[STATE_ONE:, :] * two + packs_ref[
                    source, STATE_ONE:depth, :
                ].astype(jnp.float32)

    running = running_ref[...]
    spacing = spacing_ref[...]
    running_rows = running.T
    spacing_rows = spacing.T
    wide_running = full_dot(running, spread)
    reach = reach_ref[0:1, :]
    reach_fade = jnp.exp(reach)
    reach_ref[0:1, :] = reach + wide_running[BLOCK - 1 : BLOCK]
    wide_fade = jnp.exp(wide_running)
    row = lax.broadcasted_iota(jnp.int32, (BLOCK, BLOCK), 0)
    col = lax.broadcasted_iota(jnp.int32, (BLOCK, BLOCK), 1)
    causal = row >= col
    low_lanes = lax.broadcasted_iota(jnp.int32, (BLOCK, 2 * HEAD_DIM), 1) < HEAD_DIM
    starts = (0, 2 * STATE_ONE)
    sizes = (STATE_ONE, STATE_TWO)
    pair_lanes = 2 * HEAD_DIM
    mean_shape = (pair_lanes, pair_lanes)
    mean_rows = lax.broadcasted_iota(jnp.int32, mean_shape, 0) // HEAD_DIM
    mean_cols = lax.broadcasted_iota(jnp.int32, mean_shape, 1) // HEAD_DIM
    averaging = jnp.where(mean_rows == mean_cols, 1.0 / HEAD_DIM, 0.0)
    mixed = []
    for group in range(2):
        at = starts[group]
        size = sizes[group]
        keys = key_ref[:, at : at + size]
        queries = key_ref[:, at + size : at + 2 * size]
        scores = lax.dot_general(
            queries, keys, (((1,), (1,)), ((), ())), preferred_element_type=jnp.float32
        )
        rows = slice(group * STATE_ONE, group * STATE_ONE + size)
        cols = slice(group * half, (group + 1) * half)
        entering = states_ref[0, rows, :] + entered_ref[rows, :] * reach_fade[:, cols]
        far = jnp.dot(queries, entering.astype(jnp.bfloat16), preferred_element_type=jnp.float32)
        far = far * wide_fade[:, cols]
        for pair in range(half // pair_lanes):
            lane = group * half + pair * pair_lanes
            here = slice(lane, lane + pair_lanes)
            values = conv_ref[:, here]
            zero = jnp.zeros_like(values)
            stacked = jnp.concatenate(
                [jnp.where(low_lanes, values, zero), jnp.where(low_lanes, zero, values)], axis=0
            )
            weights = []
            for head in (lane // HEAD_DIM, lane // HEAD_DIM + 1):
                gap = running[:, head : head + 1] - running_rows[head : head + 1, :]
                damping = jnp.exp(jnp.where(causal, gap, -jnp.inf))
                weights.append(
                    (scores * damping * spacing_rows[head : head + 1, :]).astype(jnp.bfloat16)
                )
            near = jnp.dot(
                jnp.concatenate(weights, axis=1), stacked, preferred_element_type=jnp.float32
            )
            summed = near + far[:, pair * pair_lanes : (pair + 1) * pair_lanes]
            summed = summed + skip_ref[:, here] * values.astype(jnp.float32)
            gated = summed * silu(gate_ref[:, here].astype(jnp.float32))
            scale = lax.rsqrt(full_dot(gated * gated, averaging) + EPSILON)
            mixed.append((gated * scale * gain_ref[:, here]).astype(jnp.bfloat16))
    mixed = jnp.concatenate(mixed, axis=1)
    out_ref[...] = jnp.dot(mixed, matrix_ref[...], preferred_element_type=jnp.float32).astype(
        jnp.bfloat16
    )


def mixer(
    values, gates, key_query, prior_rows, raw, bias, rate, extra, skip, value_taps, key_taps, gain,
    matrix,
):
    positions, lanes = values.shape
    key_width = key_query.shape[1]
    heads = raw.shape[1]
    half = lanes // 2
    blocks = positions // BLOCK
    depth = STATE_ONE + STATE_TWO
    model_width = matrix.shape[1]
    vmem = pl.BlockSpec(memory_space=pltpu.VMEM)
    conv, conv_key, running, spacing, states, pack = pl.pallas_call(
        state_kernel,
        out_shape=(
            jax.ShapeDtypeStruct((positions, lanes), jnp.bfloat16),
            jax.ShapeDtypeStruct((positions, key_width), jnp.bfloat16),
            jax.ShapeDtypeStruct((positions, heads), jnp.float32),
            jax.ShapeDtypeStruct((positions, heads), jnp.float32),
            jax.ShapeDtypeStruct((blocks, depth, half), jnp.float32),
            jax.ShapeDtypeStruct((depth + PACK_ROWS, half), jnp.bfloat16),
        ),
        in_specs=[vmem] * 9,
        out_specs=[vmem] * 6,
        scratch_shapes=[pltpu.VMEM((8 + positions, lanes + key_width), jnp.float32)],
        compiler_params=pltpu.CompilerParams(vmem_limit_bytes=32 * 1024 * 1024),
        name="mixer_states",
    )(values, key_query, prior_rows, raw, bias, rate, extra, value_taps, key_taps)
    packs = lax.all_gather(pack, "sp")
    place = lax.axis_index("sp").astype(jnp.int32).reshape(1)

    def by_block(width):
        return pl.BlockSpec((BLOCK, width), lambda k: (k, 0))

    def whole(*shape):
        return pl.BlockSpec(shape, lambda k: (0,) * len(shape))

    return pl.pallas_call(
        mix_kernel,
        grid=(blocks,),
        out_shape=jax.ShapeDtypeStruct((positions, model_width), jnp.bfloat16),
        in_specs=[
            pl.BlockSpec(memory_space=pltpu.SMEM),
            by_block(lanes),
            by_block(key_width),
            by_block(heads),
            by_block(heads),
            pl.BlockSpec((1, depth, half), lambda k: (k, 0, 0)),
            whole(*packs.shape),
            by_block(lanes),
            whole(1, lanes),
            whole(1, lanes),
            whole(lanes, model_width),
        ],
        out_specs=by_block(model_width),
        scratch_shapes=[pltpu.VMEM((depth, half), jnp.float32), pltpu.VMEM((8, lanes), jnp.float32)],
        compiler_params=pltpu.CompilerParams(vmem_limit_bytes=32 * 1024 * 1024),
        name="mixer_output",
    )(place, conv, conv_key, running, spacing, states, packs, gates, skip, gain, matrix)


def local(
    residual,
    grouped_value_heads,
    output_gate_heads,
    projected_key_query,
    raw_step_size,
    step_size_bias,
    head_decay_logarithm,
    position_extra_decay,
    head_skip_weight,
    value_kernel_taps,
    key_query_kernel,
    head_norm_gain,
    output_matrix,
    expert_norm_gain,
    expert_gate_weight,
    expert_up_weight,
    expert_down_weight,
    token_expert_choice,
    expert_output_weight,
):
    positions = grouped_value_heads.shape[0]
    lane_width = grouped_value_heads.shape[2]
    local_heads = lane_width // HEAD_DIM
    both_lanes = 2 * lane_width
    rim_depth = key_query_kernel.shape[0] - 1
    flat_values = grouped_value_heads.reshape(positions, both_lanes)
    rim_rows = jnp.concatenate(
        [flat_values[positions - rim_depth :], projected_key_query[positions - rim_depth :]], axis=1
    )
    prior_rows = passed_along(rim_rows, "sp", 1)
    both_heads = 2 * local_heads
    mix_partial = mixer(
        flat_values,
        output_gate_heads.reshape(positions, both_lanes),
        projected_key_query,
        prior_rows,
        raw_step_size.reshape(positions, both_heads),
        step_size_bias.reshape(1, both_heads),
        head_decay_logarithm.reshape(1, both_heads),
        position_extra_decay.reshape(positions, 1),
        jnp.repeat(head_skip_weight.reshape(1, both_heads), HEAD_DIM, axis=1),
        value_kernel_taps.reshape(rim_depth + 1, both_lanes),
        key_query_kernel,
        head_norm_gain.reshape(1, both_lanes),
        output_matrix.reshape(both_lanes, output_matrix.shape[2]),
    )
    rows_here = residual.shape[0]
    model_width = output_matrix.shape[2]
    mix_out = lax.psum_scatter(mix_partial, "tp", scatter_dimension=0, tiled=True).astype(jnp.float32)
    stream = (residual.astype(jnp.float32) + mix_out).astype(jnp.bfloat16)
    wide_stream = stream.astype(jnp.float32)
    normed = (
        wide_stream
        * lax.rsqrt(jnp.mean(wide_stream * wide_stream, axis=1, keepdims=True) + EPSILON)
        * expert_norm_gain[None]
    ).astype(jnp.bfloat16)
    expert_total = lax.axis_size("sp")
    capacity = 2 * rows_here // expert_total + 1
    flat_ids = token_expert_choice.reshape(-1)
    matches = (flat_ids[:, None] == jnp.arange(expert_total, dtype=jnp.int32)[None, :]).astype(
        jnp.int32
    )
    slot_rank = jnp.sum((jnp.cumsum(matches, axis=0) - matches) * matches, axis=1)
    target = flat_ids * capacity + slot_rank
    outbound = (
        jnp.zeros((expert_total * capacity, model_width), jnp.bfloat16)
        .at[target]
        .set(jnp.repeat(normed, 2, axis=0))
    )
    outbound = outbound.reshape(expert_total, capacity, model_width)
    widened = lax.all_gather(
        lax.all_to_all(outbound, "sp", split_axis=0, concat_axis=0, tiled=True),
        "tp",
        axis=0,
        tiled=True,
    )
    flat_rows = widened.reshape(-1, widened.shape[-1])
    gate_out = jnp.dot(flat_rows, expert_gate_weight[0], preferred_element_type=jnp.float32)
    up_out = jnp.dot(flat_rows, expert_up_weight[0], preferred_element_type=jnp.float32)
    hidden = (jax.nn.silu(gate_out) * up_out).astype(jnp.bfloat16)
    partial_value = jnp.dot(
        hidden, expert_down_weight[0], preferred_element_type=jnp.float32
    ).astype(jnp.bfloat16)
    partial_value = lax.optimization_barrier(
        partial_value.reshape(widened.shape[0], widened.shape[1], partial_value.shape[-1])
    ).astype(jnp.float32)
    summed = lax.psum_scatter(
        partial_value.astype(jnp.bfloat16), "tp", scatter_dimension=0, tiled=True
    )
    returned = lax.all_to_all(summed, "sp", split_axis=0, concat_axis=0, tiled=True)
    picked = jnp.take(returned.reshape(expert_total * capacity, model_width), target, axis=0)
    picked = picked.reshape(rows_here, 2, model_width).astype(jnp.float32)
    weighted = (
        expert_output_weight[:, 0:1] * picked[:, 0] + expert_output_weight[:, 1:2] * picked[:, 1]
    )
    return (wide_stream + weighted).astype(jnp.bfloat16)


def solution(mesh):
    placed = (
        P(("grp", "sp", "tp"), None),
        P(("grp", "sp"), None, "tp"),
        P(("grp", "sp"), None, "tp"),
        P(("grp", "sp"), None),
        P(("grp", "sp"), None, "tp"),
        P(None, "tp"),
        P(None, "tp"),
        P(("grp", "sp")),
        P(None, "tp"),
        P(None, None, "tp"),
        P(),
        P(None, "tp"),
        P(None, "tp", None),
        P(),
        P("sp", None, "tp"),
        P("sp", None, "tp"),
        P("sp", "tp", None),
        P(("grp", "sp", "tp"), None),
        P(("grp", "sp", "tp"), None),
    )
    return jax.shard_map(
        local, mesh=mesh, in_specs=placed, out_specs=P(("grp", "sp", "tp"), None), check_vma=False
    )
```

```python
import jax
import jax.numpy as jnp
from jax import lax
from jax.experimental import pallas as pl
from jax.experimental.pallas import tpu as pltpu
from jax.sharding import PartitionSpec as P

HEAD_DIM = 64
STATE_ONE = 64
STATE_TWO = 128
BLOCK = 128


EPSILON = 1e-06


def passed_along(shard, axis, by):
    length = lax.axis_size(axis)
    pairs = [(i, i + by) for i in range(length) if 0 <= i + by < length]
    return lax.ppermute(shard, axis, pairs)


HIGHEST = lax.Precision.HIGHEST
PACK_ROWS = 16


def full_dot(left, right):
    return jnp.dot(left, right, precision=HIGHEST, preferred_element_type=jnp.float32)


def spread_matrix(head_count):
    shape = (head_count, head_count * HEAD_DIM)
    rows = lax.broadcasted_iota(jnp.int32, shape, 0)
    lanes = lax.broadcasted_iota(jnp.int32, shape, 1)
    return (lanes // HEAD_DIM == rows).astype(jnp.float32)


def silu(value):
    return value * (1.0 / (1.0 + jnp.exp(-value)))


def state_kernel(
    value_ref, key_ref, prior_ref, raw_ref, bias_ref, rate_ref, extra_ref, value_taps_ref,
    key_taps_ref, conv_ref, conv_key_ref, running_ref, spacing_ref, states_ref, pack_ref, pad_ref,
):
    positions, lanes = value_ref.shape
    taps = value_taps_ref.shape[0]
    half = lanes // 2
    pad_ref[8 - taps + 1 : 8, :] = prior_ref[...].astype(jnp.float32)
    pad_ref[8:, :lanes] = value_ref[...].astype(jnp.float32)
    pad_ref[8:, lanes:] = key_ref[...].astype(jnp.float32)
    spacing = jax.nn.softplus(raw_ref[...].astype(jnp.float32) + bias_ref[...])
    log_decay = extra_ref[...] - jnp.exp(rate_ref[...]) * spacing
    spacing_ref[...] = spacing
    head_count = spacing.shape[1]
    spread = spread_matrix(head_count)
    row = lax.broadcasted_iota(jnp.int32, (BLOCK, BLOCK), 0)
    col = lax.broadcasted_iota(jnp.int32, (BLOCK, BLOCK), 1)
    tril = (row >= col).astype(jnp.float32)
    carried = [jnp.zeros((STATE_ONE, half), jnp.float32), jnp.zeros((STATE_TWO, half), jnp.float32)]
    total = jnp.zeros((1, lanes), jnp.float32)
    starts = (0, 2 * STATE_ONE)
    sizes = (STATE_ONE, STATE_TWO)
    value_taps = value_taps_ref[...].astype(jnp.float32)
    key_taps = key_taps_ref[...].astype(jnp.float32)
    for block in range(positions // BLOCK):
        lo = block * BLOCK
        summed = jnp.zeros((BLOCK, lanes), jnp.float32)
        key_sum = jnp.zeros((BLOCK, key_ref.shape[1]), jnp.float32)
        for tap in range(taps):
            at = lo + 8 - taps + 1 + tap
            summed = summed + pad_ref[at : at + BLOCK, :lanes] * value_taps[tap : tap + 1]
            key_sum = key_sum + pad_ref[at : at + BLOCK, lanes:] * key_taps[tap : tap + 1]
        conv = silu(summed).astype(jnp.bfloat16)
        conv_key = silu(key_sum).astype(jnp.bfloat16)
        conv_ref[lo : lo + BLOCK, :] = conv
        conv_key_ref[lo : lo + BLOCK, :] = conv_key
        running = full_dot(tril, log_decay[lo : lo + BLOCK])
        running_ref[lo : lo + BLOCK, :] = running
        end = running[BLOCK - 1 : BLOCK]
        fading = jnp.exp(end - running) * spacing[lo : lo + BLOCK]
        scaled = (conv.astype(jnp.float32) * full_dot(fading, spread)).astype(jnp.bfloat16)
        wide_end = full_dot(jnp.broadcast_to(end, (8, head_count)), spread)[:1]
        total = total + wide_end
        fade = jnp.exp(wide_end)
        for group in range(2):
            keys = conv_key[:, starts[group] : starts[group] + sizes[group]]
            at = group * STATE_ONE
            states_ref[block, at : at + sizes[group], :] = carried[group]
            state = lax.dot_general(
                keys,
                scaled[:, group * half : (group + 1) * half],
                (((0,), (0,)), ((), ())),
                preferred_element_type=jnp.float32,
            )
            carried[group] = carried[group] * fade[:, group * half : (group + 1) * half] + state
    pack_ref[:STATE_ONE, :] = carried[0].astype(jnp.bfloat16)
    pack_ref[STATE_ONE : STATE_ONE + STATE_TWO, :] = carried[1].astype(jnp.bfloat16)
    high = total.astype(jnp.bfloat16).astype(jnp.float32)
    low = total - high
    line = lax.broadcasted_iota(jnp.int32, (PACK_ROWS, half), 0)
    packed = jnp.zeros((PACK_ROWS, half), jnp.float32)
    for at, piece in enumerate((high[:, :half], high[:, half:], low[:, :half], low[:, half:])):
        packed = jnp.where(line == at, piece, packed)
    pack_ref[STATE_ONE + STATE_TWO :, :] = packed.astype(jnp.bfloat16)


def mix_kernel(
    place_ref, conv_ref, key_ref, running_ref, spacing_ref, states_ref, packs_ref, gate_ref,
    skip_ref, gain_ref, matrix_ref, out_ref, entered_ref, reach_ref,
):
    block = pl.program_id(0)
    lanes = conv_ref.shape[1]
    half = lanes // 2
    depth = STATE_ONE + STATE_TWO
    head_count = spacing_ref.shape[1]
    spread = spread_matrix(head_count)

    @pl.when(block == 0)
    def _():
        reach_ref[...] = jnp.zeros_like(reach_ref)
        entered_ref[...] = jnp.zeros_like(entered_ref)
        for source in range(packs_ref.shape[0] - 1):

            @pl.when(source < place_ref[0])
            def _():
                decay = packs_ref[source, depth:, :].astype(jnp.float32)
                one = jnp.exp(decay[0:1] + decay[2:3])
                two = jnp.exp(decay[1:2] + decay[3:4])
                entered_ref[:STATE_ONE, :] = entered_ref[:STATE_ONE, :] * one + packs_ref[
                    source, :STATE_ONE, :
                ].astype(jnp.float32)
                entered_ref[STATE_ONE:, :] = entered_ref[STATE_ONE:, :] * two + packs_ref[
                    source, STATE_ONE:depth, :
                ].astype(jnp.float32)

    running = running_ref[...]
    spacing = spacing_ref[...]
    running_rows = running.T
    spacing_rows = spacing.T
    wide_running = full_dot(running, spread)
    reach = reach_ref[0:1, :]
    reach_fade = jnp.exp(reach)
    reach_ref[0:1, :] = reach + wide_running[BLOCK - 1 : BLOCK]
    wide_fade = jnp.exp(wide_running)
    row = lax.broadcasted_iota(jnp.int32, (BLOCK, BLOCK), 0)
    col = lax.broadcasted_iota(jnp.int32, (BLOCK, BLOCK), 1)
    causal = row >= col
    low_lanes = lax.broadcasted_iota(jnp.int32, (BLOCK, 2 * HEAD_DIM), 1) < HEAD_DIM
    starts = (0, 2 * STATE_ONE)
    sizes = (STATE_ONE, STATE_TWO)
    pair_lanes = 2 * HEAD_DIM
    mean_shape = (pair_lanes, pair_lanes)
    mean_rows = lax.broadcasted_iota(jnp.int32, mean_shape, 0) // HEAD_DIM
    mean_cols = lax.broadcasted_iota(jnp.int32, mean_shape, 1) // HEAD_DIM
    averaging = jnp.where(mean_rows == mean_cols, 1.0 / HEAD_DIM, 0.0)
    mixed = []
    for group in range(2):
        at = starts[group]
        size = sizes[group]
        keys = key_ref[:, at : at + size]
        queries = key_ref[:, at + size : at + 2 * size]
        scores = lax.dot_general(
            queries, keys, (((1,), (1,)), ((), ())), preferred_element_type=jnp.float32
        )
        rows = slice(group * STATE_ONE, group * STATE_ONE + size)
        cols = slice(group * half, (group + 1) * half)
        entering = states_ref[0, rows, :] + entered_ref[rows, :] * reach_fade[:, cols]
        far = jnp.dot(queries, entering.astype(jnp.bfloat16), preferred_element_type=jnp.float32)
        far = far * wide_fade[:, cols]
        for pair in range(half // pair_lanes):
            lane = group * half + pair * pair_lanes
            here = slice(lane, lane + pair_lanes)
            values = conv_ref[:, here]
            zero = jnp.zeros_like(values)
            stacked = jnp.concatenate(
                [jnp.where(low_lanes, values, zero), jnp.where(low_lanes, zero, values)], axis=0
            )
            weights = []
            for head in (lane // HEAD_DIM, lane // HEAD_DIM + 1):
                gap = running[:, head : head + 1] - running_rows[head : head + 1, :]
                damping = jnp.exp(jnp.where(causal, gap, -jnp.inf))
                weights.append(
                    (scores * damping * spacing_rows[head : head + 1, :]).astype(jnp.bfloat16)
                )
            near = jnp.dot(
                jnp.concatenate(weights, axis=1), stacked, preferred_element_type=jnp.float32
            )
            summed = near + far[:, pair * pair_lanes : (pair + 1) * pair_lanes]
            summed = summed + skip_ref[:, here] * values.astype(jnp.float32)
            gated = summed * silu(gate_ref[:, here].astype(jnp.float32))
            scale = lax.rsqrt(full_dot(gated * gated, averaging) + EPSILON)
            mixed.append((gated * scale * gain_ref[:, here]).astype(jnp.bfloat16))
    mixed = jnp.concatenate(mixed, axis=1)
    out_ref[...] = jnp.dot(mixed, matrix_ref[...], preferred_element_type=jnp.float32).astype(
        jnp.bfloat16
    )


def mixer(
    values, gates, key_query, prior_rows, raw, bias, rate, extra, skip, value_taps, key_taps, gain,
    matrix,
):
    positions, lanes = values.shape
    key_width = key_query.shape[1]
    heads = raw.shape[1]
    half = lanes // 2
    blocks = positions // BLOCK
    depth = STATE_ONE + STATE_TWO
    model_width = matrix.shape[1]
    vmem = pl.BlockSpec(memory_space=pltpu.VMEM)
    conv, conv_key, running, spacing, states, pack = pl.pallas_call(
        state_kernel,
        out_shape=(
            jax.ShapeDtypeStruct((positions, lanes), jnp.bfloat16),
            jax.ShapeDtypeStruct((positions, key_width), jnp.bfloat16),
            jax.ShapeDtypeStruct((positions, heads), jnp.float32),
            jax.ShapeDtypeStruct((positions, heads), jnp.float32),
            jax.ShapeDtypeStruct((blocks, depth, half), jnp.float32),
            jax.ShapeDtypeStruct((depth + PACK_ROWS, half), jnp.bfloat16),
        ),
        in_specs=[vmem] * 9,
        out_specs=[vmem] * 6,
        scratch_shapes=[pltpu.VMEM((8 + positions, lanes + key_width), jnp.float32)],
        compiler_params=pltpu.CompilerParams(vmem_limit_bytes=32 * 1024 * 1024),
        name="mixer_states",
    )(values, key_query, prior_rows, raw, bias, rate, extra, value_taps, key_taps)
    packs = lax.all_gather(pack, "sp")
    place = lax.axis_index("sp").astype(jnp.int32).reshape(1)

    def by_block(width):
        return pl.BlockSpec((BLOCK, width), lambda k: (k, 0))

    def whole(*shape):
        return pl.BlockSpec(shape, lambda k: (0,) * len(shape))

    return pl.pallas_call(
        mix_kernel,
        grid=(blocks,),
        out_shape=jax.ShapeDtypeStruct((positions, model_width), jnp.bfloat16),
        in_specs=[
            pl.BlockSpec(memory_space=pltpu.SMEM),
            by_block(lanes),
            by_block(key_width),
            by_block(heads),
            by_block(heads),
            pl.BlockSpec((1, depth, half), lambda k: (k, 0, 0)),
            whole(*packs.shape),
            by_block(lanes),
            whole(1, lanes),
            whole(1, lanes),
            whole(lanes, model_width),
        ],
        out_specs=by_block(model_width),
        scratch_shapes=[pltpu.VMEM((depth, half), jnp.float32), pltpu.VMEM((8, lanes), jnp.float32)],
        compiler_params=pltpu.CompilerParams(vmem_limit_bytes=32 * 1024 * 1024),
        name="mixer_output",
    )(place, conv, conv_key, running, spacing, states, packs, gates, skip, gain, matrix)


def local(
    residual,
    grouped_value_heads,
    output_gate_heads,
    projected_key_query,
    raw_step_size,
    step_size_bias,
    head_decay_logarithm,
    position_extra_decay,
    head_skip_weight,
    value_kernel_taps,
    key_query_kernel,
    head_norm_gain,
    output_matrix,
    expert_norm_gain,
    expert_gate_weight,
    expert_up_weight,
    expert_down_weight,
    token_expert_choice,
    expert_output_weight,
):
    positions = grouped_value_heads.shape[0]
    lane_width = grouped_value_heads.shape[2]
    local_heads = lane_width // HEAD_DIM
    both_lanes = 2 * lane_width
    rim_depth = key_query_kernel.shape[0] - 1
    flat_values = grouped_value_heads.reshape(positions, both_lanes)
    rim_rows = jnp.concatenate(
        [flat_values[positions - rim_depth :], projected_key_query[positions - rim_depth :]], axis=1
    )
    prior_rows = passed_along(rim_rows, "sp", 1)
    both_heads = 2 * local_heads
    mix_partial = mixer(
        flat_values,
        output_gate_heads.reshape(positions, both_lanes),
        projected_key_query,
        prior_rows,
        raw_step_size.reshape(positions, both_heads),
        step_size_bias.reshape(1, both_heads),
        head_decay_logarithm.reshape(1, both_heads),
        position_extra_decay.reshape(positions, 1),
        jnp.repeat(head_skip_weight.reshape(1, both_heads), HEAD_DIM, axis=1),
        value_kernel_taps.reshape(rim_depth + 1, both_lanes),
        key_query_kernel,
        head_norm_gain.reshape(1, both_lanes),
        output_matrix.reshape(both_lanes, output_matrix.shape[2]),
    )
    rows_here = residual.shape[0]
    model_width = output_matrix.shape[2]
    mix_out = lax.psum_scatter(mix_partial, "tp", scatter_dimension=0, tiled=True).astype(jnp.float32)
    stream = (residual.astype(jnp.float32) + mix_out).astype(jnp.bfloat16)
    wide_stream = stream.astype(jnp.float32)
    normed = (
        wide_stream
        * lax.rsqrt(jnp.mean(wide_stream * wide_stream, axis=1, keepdims=True) + EPSILON)
        * expert_norm_gain[None]
    ).astype(jnp.bfloat16)
    expert_total = lax.axis_size("sp")
    capacity = -(-(2 * rows_here // expert_total + 1) // 8) * 8
    first_rows = capacity // 16 * 8
    flat_ids = token_expert_choice.reshape(-1)
    matches = (flat_ids[:, None] == jnp.arange(expert_total, dtype=jnp.int32)[None, :]).astype(
        jnp.int32
    )
    slot_rank = jnp.sum((jnp.cumsum(matches, axis=0) - matches) * matches, axis=1)
    target = flat_ids * capacity + slot_rank
    outbound = (
        jnp.zeros((expert_total * capacity, model_width), jnp.bfloat16)
        .at[target]
        .set(jnp.repeat(normed, 2, axis=0))
    )
    outbound = outbound.reshape(expert_total, capacity, model_width)
    sent = [
        lax.all_to_all(piece, "sp", split_axis=0, concat_axis=0, tiled=True)
        for piece in (outbound[:, :first_rows], outbound[:, first_rows:])
    ]
    widened = [lax.all_gather(piece, "tp", axis=0, tiled=True) for piece in sent]
    summed = []
    for piece in widened:
        flat_rows = piece.reshape(-1, model_width)
        gate_out = jnp.dot(flat_rows, expert_gate_weight[0], preferred_element_type=jnp.float32)
        up_out = jnp.dot(flat_rows, expert_up_weight[0], preferred_element_type=jnp.float32)
        hidden = (jax.nn.silu(gate_out) * up_out).astype(jnp.bfloat16)
        partial_value = jnp.dot(
            hidden, expert_down_weight[0], preferred_element_type=jnp.float32
        ).astype(jnp.bfloat16)
        summed.append(
            lax.psum_scatter(
                partial_value.reshape(piece.shape), "tp", scatter_dimension=0, tiled=True
            )
        )
    returned = jnp.concatenate(
        [lax.all_to_all(piece, "sp", split_axis=0, concat_axis=0, tiled=True) for piece in summed],
        axis=1,
    )
    picked = jnp.take(returned.reshape(expert_total * capacity, model_width), target, axis=0)
    picked = picked.reshape(rows_here, 2, model_width).astype(jnp.float32)
    weighted = (
        expert_output_weight[:, 0:1] * picked[:, 0] + expert_output_weight[:, 1:2] * picked[:, 1]
    )
    return (wide_stream + weighted).astype(jnp.bfloat16)


def solution(mesh):
    placed = (
        P(("grp", "sp", "tp"), None),
        P(("grp", "sp"), None, "tp"),
        P(("grp", "sp"), None, "tp"),
        P(("grp", "sp"), None),
        P(("grp", "sp"), None, "tp"),
        P(None, "tp"),
        P(None, "tp"),
        P(("grp", "sp")),
        P(None, "tp"),
        P(None, None, "tp"),
        P(),
        P(None, "tp"),
        P(None, "tp", None),
        P(),
        P("sp", None, "tp"),
        P("sp", None, "tp"),
        P("sp", "tp", None),
        P(("grp", "sp", "tp"), None),
        P(("grp", "sp", "tp"), None),
    )
    return jax.shard_map(
        local, mesh=mesh, in_specs=placed, out_specs=P(("grp", "sp", "tp"), None), check_vma=False
    )
```
